32 devices in a mesh: grp: 2 (over y), fs: 8 (over z, core), tp: 2 (over x).
Axes of the slice: x: 2, y: 2, z: 4, core: 2. Of those that a mesh axis runs over, the one named last changes fastest.
Arguments:
- prompt: bfloat16 [6144, 2048], P(('grp', 'fs')), parts along dimension 0, may hold values from -6 to 6
- routes: int32 [6144, 4], P(('grp', 'fs')), parts along dimension 0, may hold values from 0 to 7, all different within a row; in each aligned block of 384 rows (0 to 383, 384 to 767, ...) at most 240 rows name the same one
- route_weight: float32 [6144, 4], P(('grp', 'fs')), parts along dimension 0, may hold values from 0.2 to 1
- norm_gain: float32 [2048], P('fs'), may hold values from 0.1 to 1.9
- gate_train: float32 [8, 2048, 1024], P(None, 'fs', 'tp'), may hold values from -0.4 to 0.4
- up_train: float32 [8, 2048, 1024], P(None, 'fs', 'tp'), may hold values from -0.4 to 0.4
- down_train: float32 [8, 1024, 2048], P(None, 'fs', 'tp'), may hold values from -0.07 to 0.07
Outputs:
- gate_serve: bfloat16 [16, 2048, 1024], P(('grp', 'fs'), None, 'tp'), parts along dimension 0
- up_serve: bfloat16 [16, 2048, 1024], P(('grp', 'fs'), None, 'tp'), parts along dimension 0
- down_serve: bfloat16 [16, 1024, 2048], P(('grp', 'fs'), 'tp'), parts along dimension 0
- mixed: bfloat16 [6144, 2048], P(('grp', 'fs'), 'tp'), parts along dimension 0
The draws below stay inside these ranges and needn't reach their ends.
There are 2 independent parts, one for each index of `grp`. The reference program is written for one: setup_inputs(seed, part) draws one part's arguments, and reference() takes and returns one part's arrays. A program takes and returns all parts, laid end to end along the dimension named above; an argument that names none is the same for every part. Nothing has to cross between parts.
Inputs may be any that keep to these rules, and one draw needn't show every extreme that they name: `routes`: each row names 4 different experts. Among the rows of one index of fs no expert is named more than 240 times, a bound that some block reaches on some index.
All inputs are finite; a program needn't handle non-finite values.
Results may differ from the reference program's by a relative error of at most 0.012.
Values may be sent and summed in bfloat16 or wider, within the bound.
A program may use at most 128 MiB of HBM per device.

```python
import math
import jax
import jax.numpy as jnp
import numpy as np
from jax import lax

D = 2048
FF = 1024
TOP = 4
TOK_DEV = 384
EXPERTS = 8
CAP = 240
TOKENS = 3072
N_FS = 8
N_TP = 2


def shard_levels(stream_key, extent, shards, least, top_value):
    loudness, own = 1.0, jax.random.fold_in(stream_key, 6)
    for dim, parts in shards:
        heights = jnp.exp(jax.random.uniform(jax.random.fold_in(own, dim), (parts,), jnp.float32, least / len(shards), top_value / len(shards)))
        loudness = loudness * jnp.repeat(heights, extent[dim] // parts).reshape([-1 if axis == dim else 1 for axis in range(len(extent))])
    return loudness


def deal_out(own_key, own, number, rows, number_of, top, reach, slope):
    sequence = jax.random.permutation(own_key, number_of)
    packed, common = portions_of(number_of, rows * top, reach, slope, True), portions_of(number_of, rows * top, reach, slope, False)
    places = jnp.arange(number_of)

    def named(lengths, turn):
        used = int((lengths > 0).sum())
        fixed = max(1, used // 4)
        passed = fixed + (places - fixed + turn * (used - fixed)) % max(1, number_of - fixed)
        return jnp.zeros((number_of,), jnp.int32).at[sequence[jnp.where(places < fixed, places, passed)]].set(jnp.asarray(lengths, jnp.int32))

    lengths = jnp.where(number % 4 == 0, named(packed, number // 4), named(common, number - number // 4 - 1))
    mixed = jax.random.permutation(jax.random.fold_in(own, 3), number_of)
    donor, receiver = mixed[0:number_of // 2 * 2:2], mixed[1:number_of // 2 * 2:2]
    slack = jnp.minimum(lengths[donor] - 1, reach - lengths[receiver]) // 2
    slack = jnp.where((donor == sequence[0]) | (receiver == sequence[0]) | (lengths[receiver] == 0), 0, jnp.maximum(slack, 0))
    passed = jax.random.randint(jax.random.fold_in(own, 4), (number_of // 2,), 0, 1 << 20) % (slack + 1)
    lengths = lengths.at[donor].add(-passed).at[receiver].add(passed)
    members = jnp.searchsorted(jnp.cumsum(lengths), jnp.arange(rows * top), side="right").astype(jnp.int32)
    grid = members.reshape(top, rows).T
    grid = grid[jax.random.permutation(jax.random.fold_in(own, 1), rows)]
    turn = jax.random.randint(jax.random.fold_in(own, 2), (rows, 1), 0, top)
    return jnp.take_along_axis(grid, (jnp.arange(top)[None, :] + turn) % top, axis=1)


def portions_of(count, total, limit, slope, full):
    portions = [(1 << 20) // math.isqrt(rank ** slope) + 1 for rank in range(1, count + 1)]
    largest = limit if full else min(limit, max(-(-total // count), total * portions[0] // sum(portions)))
    least = 1 if total - largest >= count - 1 else 0
    counts, rest = [largest] + [least] * (count - 1), total - largest - least * (count - 1)
    while rest > 0:
        candidates = [i for i in range(1, count) if counts[i] < largest] or [i for i in range(1, count) if counts[i] < limit]
        mass, budget = sum([portions[i] for i in candidates]), rest
        for i in candidates:
            more = min(limit - counts[i], max(1, budget * portions[i] // mass), rest)
            counts[i] = counts[i] + more
            rest = rest - more
    return np.array(counts)


def scatter_about(rng, dims, scale, limit, cuts=(), held_as=jnp.bfloat16):
    values = jax.random.normal(rng, dims, jnp.float32) * scale
    if len(cuts) > 0:
        values = shard_levels(rng, dims, cuts, -0.22, 0.18) * values
    return jnp.clip(values, min=-limit, max=limit).astype(held_as)


def setup_inputs(seed: int = 0, part: int = 0) -> dict:
    keys = jax.random.split(jax.random.key(seed), 8)
    part_splits = jax.random.split(jax.random.fold_in(keys[7], part), 8)
    prompt = scatter_about(part_splits[0], (TOKENS, D), 1.0, 6.0, ((0, 8),))
    routes_keys = jax.random.split(jax.random.fold_in(part_splits[1], 1), TOKENS // TOK_DEV)
    routes_turns = jax.random.permutation(jax.random.fold_in(part_splits[1], 3), TOKENS // TOK_DEV)
    routes = jax.vmap(lambda own, number: deal_out(jax.random.fold_in(part_splits[1], 2), own, number, TOK_DEV, EXPERTS, TOP, CAP, 1))(routes_keys, routes_turns).reshape((TOKENS, TOP))
    route_weight = jnp.clip(jnp.exp(math.log(1.0) - 1.609438 * jax.random.uniform(part_splits[2], (TOKENS, TOP), jnp.float32) ** shard_levels(part_splits[2], (TOKENS, TOP), ((0, 8),), -0.2, 0.2)), 0.2, 1.0)
    norm_gain = jnp.clip(1.0 + 0.18 * jax.random.normal(keys[3], (D,), jnp.float32), 0.1, 1.9)
    gate_train = scatter_about(keys[4], (EXPERTS, D, FF), 0.055, 0.4, ((1, 8), (2, 2)), jnp.float32)
    up_train = scatter_about(keys[5], (EXPERTS, D, FF), 0.055, 0.4, ((1, 8), (2, 2)), jnp.float32)
    down_train = scatter_about(keys[6], (EXPERTS, FF, D), 0.01, 0.07, ((1, 8), (2, 2)), jnp.float32)
    return {"prompt": prompt, "routes": routes, "route_weight": route_weight, "norm_gain": norm_gain, "gate_train": gate_train, "up_train": up_train, "down_train": down_train}


LIMIT = 7.0
ALPHA = 1.702
EPS = 1e-06

def expert_apply(rows, gate_one, up_one, down_one):
    gate_pre = jnp.dot(rows, gate_one, preferred_element_type=jnp.float32)
    up_pre = jnp.dot(rows, up_one, preferred_element_type=jnp.float32)
    gate_pre = jnp.minimum(gate_pre, LIMIT)
    up_pre = jnp.clip(up_pre, -LIMIT, LIMIT)
    hidden = ((up_pre + 1.0) * gate_pre * jax.nn.sigmoid(ALPHA * gate_pre)).astype(jnp.bfloat16)
    width = hidden.shape[1] // N_TP
    total = jnp.zeros((rows.shape[0], down_one.shape[1]), jnp.float32)
    for block in range(N_TP):
        part = jnp.dot(hidden[:, block * width:(block + 1) * width], down_one[block * width:(block + 1) * width], preferred_element_type=jnp.float32).astype(jnp.bfloat16)
        part = lax.optimization_barrier(part)
        total = total + part.astype(jnp.float32)
    return total.astype(jnp.bfloat16)

def reference(prompt, routes, route_weight, norm_gain, gate_train, up_train, down_train):
    gate_serve = (norm_gain[None, :, None] * gate_train).astype(jnp.bfloat16)
    up_serve = (norm_gain[None, :, None] * up_train).astype(jnp.bfloat16)
    down_serve = down_train.astype(jnp.bfloat16)
    values = prompt.astype(jnp.float32)
    normed = (values * lax.rsqrt(lax.optimization_barrier(jnp.mean(values * values, axis=-1, keepdims=True)) + EPS)).astype(jnp.bfloat16)
    flat_expert = routes.reshape(-1).astype(jnp.int32)
    flat_weight = route_weight.reshape(-1)
    most = N_FS * CAP
    experts = gate_serve.shape[0]

    def one_expert(carry, expert):
        chosen = flat_expert == expert
        picks = jnp.nonzero(chosen, size=most, fill_value=0)[0].astype(jnp.int32)
        live = jnp.arange(most, dtype=jnp.int32) < jnp.sum(chosen.astype(jnp.int32))
        token = (picks // TOP).astype(jnp.int32)
        rows = normed[token]
        result = expert_apply(rows, gate_serve[expert], up_serve[expert], down_serve[expert])
        scale = jnp.where(live, flat_weight[picks], 0.0).astype(jnp.float32)
        carry = carry.at[token].add(result.astype(jnp.float32) * scale[:, None])
        return (carry, None)
    start = jnp.zeros(normed.shape, jnp.float32)
    total, unused = lax.scan(one_expert, start, jnp.arange(experts, dtype=jnp.int32))
    return (gate_serve, up_serve, down_serve, total.astype(jnp.bfloat16))
```

```python
import jax
import jax.numpy as jnp
from jax import lax
from jax.sharding import PartitionSpec as P

LIMIT = 7.0
ALPHA = 1.702
EPS = 1e-06


def shards(prompt, routes, route_weight, norm_gain, gate_train, up_train, down_train):
    tp = lax.axis_size("tp")
    experts = gate_train.shape[0]
    tok_rows, width = prompt.shape
    values = prompt.astype(jnp.float32)
    normed = (values * lax.rsqrt(jnp.mean(values * values, axis=-1, keepdims=True) + EPS)).astype(
        jnp.bfloat16
    )
    lanes = jnp.arange(experts, dtype=jnp.int32)
    scale = jnp.sum(
        jnp.where(routes[:, :, None] == lanes[None, None, :], route_weight[:, :, None], 0.0), axis=1
    )
    scale = lax.all_to_all(scale.T, "fs", split_axis=0, concat_axis=0, tiled=True)
    scale = scale.reshape(-1, 1)
    tokens = lax.all_gather(normed, "fs", axis=0, tiled=True)

    gain = norm_gain[None, :, None]
    gate_mine = lax.all_to_all(
        (gain * gate_train).astype(jnp.bfloat16), "fs", split_axis=0, concat_axis=0, tiled=True
    ).reshape(width, -1)
    up_mine = lax.all_to_all(
        (gain * up_train).astype(jnp.bfloat16), "fs", split_axis=0, concat_axis=0, tiled=True
    ).reshape(width, -1)
    down_rows = lax.all_to_all(
        down_train.astype(jnp.bfloat16), "fs", split_axis=0, concat_axis=0, tiled=True
    )
    down_rows = down_rows.reshape(-1, down_rows.shape[2])
    cols = down_rows.shape[1]
    own = gate_mine.shape[1]
    down_mine = lax.all_to_all(down_rows, "tp", split_axis=0, concat_axis=0, tiled=True)
    down_mine = down_mine.reshape(tp, own, cols).transpose(1, 0, 2).reshape(own, tp * cols)

    gate_pre = jnp.minimum(
        jnp.dot(tokens, gate_mine, preferred_element_type=jnp.float32), LIMIT
    )
    up_pre = jnp.clip(
        jnp.dot(tokens, up_mine, preferred_element_type=jnp.float32), -LIMIT, LIMIT
    )
    hidden = ((up_pre + 1.0) * gate_pre * jax.nn.sigmoid(ALPHA * gate_pre)).astype(jnp.bfloat16)
    pieces = lax.all_gather(hidden, "tp", axis=0, tiled=True)
    total = jnp.zeros((hidden.shape[0], cols), jnp.float32)
    for index in range(tp):
        total = total + jnp.dot(
            pieces[index * hidden.shape[0] : (index + 1) * hidden.shape[0]],
            down_rows[index * own : (index + 1) * own],
            preferred_element_type=jnp.float32,
        )
    weighted = (total * scale).astype(jnp.bfloat16)
    mixed = lax.psum_scatter(weighted, "fs", scatter_dimension=0, tiled=True)
    return (gate_mine[None], up_mine[None], down_mine[None], mixed)


def solution(mesh):
    return jax.shard_map(
        shards,
        mesh=mesh,
        in_specs=(
            P(("grp", "fs"), None),
            P(("grp", "fs"), None),
            P(("grp", "fs"), None),
            P("fs"),
            P(None, "fs", "tp"),
            P(None, "fs", "tp"),
            P(None, "fs", "tp"),
        ),
        out_specs=(
            P(("grp", "fs"), None, "tp"),
            P(("grp", "fs"), None, "tp"),
            P(("grp", "fs"), "tp", None),
            P(("grp", "fs"), "tp"),
        ),
        check_vma=False,
    )
```

```python
import functools

import jax
import jax.numpy as jnp
from jax import lax
from jax.experimental import pallas as pl
from jax.experimental.pallas import tpu as pltpu
from jax.sharding import PartitionSpec as P

LIMIT = 7.0
ALPHA = 1.702
EPS = 1e-06
MESH = pl.DeviceIdType.MESH


def exchange(
    sizes,
    tok_in,
    gate_in,
    up_in,
    down_in,
    tok,
    gate,
    up,
    down,
    recv_w,
    send_w,
    recv_t,
    send_up,
    send_dn,
    send_pt,
    local,
):
    G, F, T = sizes
    g, f, t = lax.axis_index("grp"), lax.axis_index("fs"), lax.axis_index("tp")
    barrier = pltpu.get_barrier_semaphore()
    for axis, here, count in (("fs", f, F), ("grp", g, G), ("tp", t, T)):
        for s in range(1, count):
            pl.semaphore_signal(
                barrier, inc=1, device_id={axis: lax.rem(here + s, count)}, device_id_type=MESH
            )
    pl.semaphore_wait(barrier, F + G + T - 3)

    def remote(src, dst, send, recv, **where):
        return pltpu.make_async_remote_copy(
            src_ref=src, dst_ref=dst, send_sem=send, recv_sem=recv, device_id=where,
            device_id_type=MESH,
        )

    mats = ((gate_in, gate), (up_in, up), (down_in, down))

    def rows_of(m, src, gg, tt):
        block = mats[m][0].shape[1]
        piece = block // G
        start = (tt * F + src) * block + gg * piece
        return mats[m][1].at[pl.ds(pl.multiple_of(start, piece), piece)]

    def sent_piece(m, expert):
        piece = mats[m][0].shape[1] // G
        return mats[m][0].at[expert, pl.ds(pl.multiple_of(g * piece, piece), piece)]

    def wait_piece(m, src, gg, tt):
        ref = rows_of(m, src, gg, tt)
        remote(ref, ref, send_w.at[m], recv_w.at[m, src, gg, tt], fs=lax.rem(f + 1, F)).wait_recv()

    def pass_on(m, src, gg, tt, **where):
        ref = rows_of(m, src, gg, tt)
        remote(ref, ref, send_w.at[m], recv_w.at[m, src, gg, tt], **where).start()

    rows = tok_in.shape[0]

    def block_of(src):
        return tok.at[pl.ds(pl.multiple_of(src * rows, rows), rows)]

    Z = F // 2
    z, core = f // 2, lax.rem(f, 2)
    partner = f + 1 - 2 * core

    own = [pltpu.make_async_copy(tok_in, block_of(f), local.at[3])]
    for m in range(3):
        own.append(pltpu.make_async_copy(sent_piece(m, f), rows_of(m, f, g, t), local.at[m]))
    for copy in own:
        copy.start()

    for m in range(3):

        @pl.loop(1, F)
        def _(s, m=m):
            to = lax.rem(f + s, F)
            remote(
                sent_piece(m, to), rows_of(m, f, g, t), send_w.at[m], recv_w.at[m, f, g, t], fs=to
            ).start()

    def tok_copy(src_ref, src, kind):
        sems, to = ((send_up, f + 2), (send_dn, f - 2), (send_pt, partner))[kind]
        return remote(src_ref, block_of(src), sems.at[src], recv_t.at[src], fs=to)

    @pl.when(z < Z - 1)
    def _():
        tok_copy(tok_in, f, 0).start()

    @pl.when(z > 0)
    def _():
        tok_copy(tok_in, f, 1).start()

    tok_copy(tok_in, f, 2).start()

    def first(m, src):
        for dg in range(1, G):
            pass_on(m, src, g, t, grp=lax.rem(g + dg, G))
        for dt in range(1, T):
            pass_on(m, src, g, t, tp=lax.rem(t + dt, T))

    def phase1(m):
        own[m + 1].wait()
        first(m, f)

        @pl.loop(1, F)
        def _(s):
            src = lax.rem(f - s + F, F)
            wait_piece(m, src, g, t)
            first(m, src)

    def phase2(m):
        @pl.loop(0, F)
        def _(s):
            src = lax.rem(f - s + F, F)
            even = lax.rem(src, 2) == 0
            for dg in range(1, G):
                gg = lax.rem(g + dg, G)
                wait_piece(m, src, gg, t)

                @pl.when(even)
                def _():
                    for dt in range(1, T):
                        pass_on(m, src, gg, t, tp=lax.rem(t + dt, T))

            for dt in range(1, T):
                tt = lax.rem(t + dt, T)
                wait_piece(m, src, g, tt)

                @pl.when(jnp.logical_not(even))
                def _():
                    for dg in range(1, G):
                        pass_on(m, src, g, tt, grp=lax.rem(g + dg, G))

    def chain(low, high):
        @pl.loop(low, high)
        def _(d):
            @pl.when(z >= d)
            def _():
                src = f - 2 * d
                tok_copy(block_of(src), src, 2).wait_recv()

                @pl.when(z < Z - 1)
                def _():
                    tok_copy(block_of(src), src, 0).start()

                tok_copy(block_of(src), src, 2).start()

            @pl.when(z + d < Z)
            def _():
                src = f + 2 * d
                tok_copy(block_of(src), src, 2).wait_recv()

                @pl.when(z > 0)
                def _():
                    tok_copy(block_of(src), src, 1).start()

                tok_copy(block_of(src), src, 2).start()

    phase1(0)
    phase1(1)
    phase2(0)
    phase1(2)
    chain(1, 2)
    phase2(1)
    chain(2, 3)
    phase2(2)
    chain(3, Z)

    for m in range(3):

        @pl.loop(0, F)
        def _(src, m=m):
            for dg in range(1, G):
                for dt in range(1, T):
                    wait_piece(m, src, lax.rem(g + dg, G), lax.rem(t + dt, T))

        out = mats[m][1]
        sent = out.at[pl.ds(0, out.shape[0] - mats[m][0].shape[1] // G)]
        remote(sent, sent, send_w.at[m], recv_w.at[m, 0, 0, 0], fs=lax.rem(f + 1, F)).wait_send()

    own[0].wait()

    @pl.loop(0, Z)
    def _(zz):
        src = 2 * zz + core
        other = 2 * zz + 1 - core
        tok_copy(block_of(other), other, 2).wait_recv()
        tok_copy(block_of(src), src, 2).wait_send()

        @pl.when(jnp.logical_and(zz <= z, z < Z - 1))
        def _():
            tok_copy(block_of(src), src, 0).wait_send()

        @pl.when(jnp.logical_and(zz >= z, z > 0))
        def _():
            tok_copy(block_of(src), src, 1).wait_send()


def gathered(mesh, tok_in, gate_in, up_in, down_in):
    G, F, T = (mesh.shape[name] for name in ("grp", "fs", "tp"))
    full = [
        jax.ShapeDtypeStruct((T * F * w.shape[1], w.shape[2]), w.dtype)
        for w in (gate_in, up_in, down_in)
    ]
    return pl.pallas_call(
        functools.partial(exchange, (G, F, T)),
        out_shape=[jax.ShapeDtypeStruct((F * tok_in.shape[0], tok_in.shape[1]), tok_in.dtype)]
        + full,
        in_specs=[pl.BlockSpec(memory_space=pl.ANY)] * 4,
        out_specs=[pl.BlockSpec(memory_space=pltpu.VMEM)] * 4,
        scratch_shapes=[
            pltpu.SemaphoreType.DMA((3, F, G, T)),
            pltpu.SemaphoreType.DMA((3,)),
            pltpu.SemaphoreType.DMA((F,)),
            pltpu.SemaphoreType.DMA((F,)),
            pltpu.SemaphoreType.DMA((F,)),
            pltpu.SemaphoreType.DMA((F,)),
            pltpu.SemaphoreType.DMA((4,)),
        ],
        compiler_params=pltpu.CompilerParams(
            collective_id=0, has_side_effects=True, vmem_limit_bytes=40 * 1024 * 1024
        ),
    )(tok_in, gate_in, up_in, down_in)


def shards(mesh, prompt, routes, route_weight, norm_gain, gate_train, up_train, down_train):
    T, F = mesh.shape["tp"], mesh.shape["fs"]
    t = lax.axis_index("tp")
    experts = gate_train.shape[0]
    tok_rows, width = prompt.shape
    part = tok_rows // T
    values = lax.dynamic_slice_in_dim(prompt, t * part, part, 0).astype(jnp.float32)
    normed = (values * lax.rsqrt(jnp.mean(values * values, axis=-1, keepdims=True) + EPS)).astype(
        jnp.bfloat16
    )
    lanes = jnp.arange(experts, dtype=jnp.int32)
    routes = lax.dynamic_slice_in_dim(routes, t * part, part, 0)
    route_weight = lax.dynamic_slice_in_dim(route_weight, t * part, part, 0)
    scale = jnp.sum(
        jnp.where(routes[:, :, None] == lanes[None, None, :], route_weight[:, :, None], 0.0), axis=1
    )
    scale = lax.all_to_all(scale.T, "fs", split_axis=0, concat_axis=0, tiled=True)
    scale = scale.reshape(-1, 1)

    gain = norm_gain[None, :, None]
    tokens, gate, up, down = gathered(
        mesh,
        normed,
        (gain * gate_train).astype(jnp.bfloat16),
        (gain * up_train).astype(jnp.bfloat16),
        down_train.astype(jnp.bfloat16),
    )
    gate, up, down = (w.reshape(T, w.shape[0] // T, w.shape[1]) for w in (gate, up, down))
    own = gate.shape[2]
    gate_mine = lax.dynamic_slice_in_dim(gate, t, 1, 0)
    up_mine = lax.dynamic_slice_in_dim(up, t, 1, 0)
    down_mine = lax.dynamic_slice_in_dim(down, t * own, own, 1)
    down_mine = down_mine.transpose(1, 0, 2).reshape(1, own, -1)

    hidden = []
    for i in range(T):
        gate_pre = jnp.dot(tokens, gate[i], preferred_element_type=jnp.float32)
        up_pre = jnp.dot(tokens, up[i], preferred_element_type=jnp.float32)
        gate_pre = jnp.minimum(gate_pre, LIMIT)
        up_pre = jnp.clip(up_pre, -LIMIT, LIMIT)
        hidden.append(
            ((up_pre + 1.0) * gate_pre * jax.nn.sigmoid(ALPHA * gate_pre)).astype(jnp.bfloat16)
        )
    hidden = jnp.concatenate(hidden, axis=1)
    weighted = [
        (jnp.dot(hidden, down[i], preferred_element_type=jnp.float32) * scale).astype(jnp.bfloat16)
        for i in range(T)
    ]
    weighted = jnp.concatenate(weighted, axis=1)
    summed = lax.psum_scatter(weighted, "fs", scatter_dimension=0, tiled=True)
    mixed = lax.all_to_all(summed, "tp", split_axis=1, concat_axis=0, tiled=True)
    return (gate_mine, up_mine, down_mine, mixed)


def solution(mesh):
    return jax.shard_map(
        functools.partial(shards, mesh),
        mesh=mesh,
        in_specs=(
            P(("grp", "fs"), None),
            P(("grp", "fs"), None),
            P(("grp", "fs"), None),
            P("fs"),
            P(None, "fs", "tp"),
            P(None, "fs", "tp"),
            P(None, "fs", "tp"),
        ),
        out_specs=(
            P(("grp", "fs"), None, "tp"),
            P(("grp", "fs"), None, "tp"),
            P(("grp", "fs"), "tp", None),
            P(("grp", "fs"), "tp"),
        ),
        check_vma=False,
    )
```

```python
import functools

import jax
import jax.numpy as jnp
from jax import lax
from jax.experimental import pallas as pl
from jax.experimental.pallas import tpu as pltpu
from jax.sharding import PartitionSpec as P

LIMIT = 7.0
ALPHA = 1.702
EPS = 1e-06
MESH = pl.DeviceIdType.MESH


def exchange(
    sizes,
    scale_in,
    tok_in,
    gate_in,
    up_in,
    down_in,
    scale,
    tok,
    gate,
    up,
    down,
    recv_w,
    send_w,
    recv_t,
    send_up,
    send_dn,
    send_pt,
    recv_s,
    send_s,
    local,
):
    G, F, T = sizes
    g, f, t = lax.axis_index("grp"), lax.axis_index("fs"), lax.axis_index("tp")
    barrier = pltpu.get_barrier_semaphore()
    for axis, here, count in (("fs", f, F), ("grp", g, G), ("tp", t, T)):
        for s in range(1, count):
            pl.semaphore_signal(
                barrier, inc=1, device_id={axis: lax.rem(here + s, count)}, device_id_type=MESH
            )
    pl.semaphore_wait(barrier, F + G + T - 3)

    def remote(src, dst, send, recv, **where):
        return pltpu.make_async_remote_copy(
            src_ref=src, dst_ref=dst, send_sem=send, recv_sem=recv, device_id=where,
            device_id_type=MESH,
        )

    mats = ((gate_in, gate), (up_in, up), (down_in, down))

    def rows_of(m, src, gg, tt):
        block = mats[m][0].shape[1]
        piece = block // G
        start = (tt * F + src) * block + gg * piece
        return mats[m][1].at[pl.ds(pl.multiple_of(start, piece), piece)]

    def sent_piece(m, expert):
        piece = mats[m][0].shape[1] // G
        return mats[m][0].at[expert, pl.ds(pl.multiple_of(g * piece, piece), piece)]

    def wait_piece(m, src, gg, tt):
        ref = rows_of(m, src, gg, tt)
        remote(ref, ref, send_w.at[m], recv_w.at[m, src, gg, tt], fs=lax.rem(f + 1, F)).wait_recv()

    def pass_on(m, src, gg, tt, **where):
        ref = rows_of(m, src, gg, tt)
        remote(ref, ref, send_w.at[m], recv_w.at[m, src, gg, tt], **where).start()

    rows = tok_in.shape[0]

    def block_of(src):
        return tok.at[pl.ds(pl.multiple_of(src * rows, rows), rows)]

    Z = F // 2
    z, core = f // 2, lax.rem(f, 2)
    partner = f + 1 - 2 * core

    own_scale = pltpu.make_async_copy(scale_in.at[f], scale.at[f], local.at[4])
    own_scale.start()

    def scale_copy(to, src):
        return remote(scale_in.at[to], scale.at[src], send_s.at[to], recv_s.at[src], fs=to)

    own = [pltpu.make_async_copy(tok_in, block_of(f), local.at[3])]
    for m in range(3):
        own.append(pltpu.make_async_copy(sent_piece(m, f), rows_of(m, f, g, t), local.at[m]))
    for copy in own:
        copy.start()

    @pl.loop(1, F)
    def _(s):
        scale_copy(lax.rem(f + s, F), f).start()

    for m in range(3):

        @pl.loop(1, F)
        def _(s, m=m):
            to = lax.rem(f + s, F)
            remote(
                sent_piece(m, to), rows_of(m, f, g, t), send_w.at[m], recv_w.at[m, f, g, t], fs=to
            ).start()

    def tok_copy(src_ref, src, kind):
        sems, to = ((send_up, f + 2), (send_dn, f - 2), (send_pt, partner))[kind]
        return remote(src_ref, block_of(src), sems.at[src], recv_t.at[src], fs=to)

    @pl.when(z < Z - 1)
    def _():
        tok_copy(tok_in, f, 0).start()

    @pl.when(z > 0)
    def _():
        tok_copy(tok_in, f, 1).start()

    tok_copy(tok_in, f, 2).start()

    def first(m, src):
        for dg in range(1, G):
            pass_on(m, src, g, t, grp=lax.rem(g + dg, G))
        for dt in range(1, T):
            pass_on(m, src, g, t, tp=lax.rem(t + dt, T))

    def phase1(m):
        own[m + 1].wait()
        first(m, f)

        @pl.loop(1, F)
        def _(s):
            src = lax.rem(f - s + F, F)
            wait_piece(m, src, g, t)
            first(m, src)

    def phase2(m):
        @pl.loop(0, F)
        def _(s):
            src = lax.rem(f - s + F, F)
            even = lax.rem(src, 2) == 0
            for dg in range(1, G):
                gg = lax.rem(g + dg, G)
                wait_piece(m, src, gg, t)

                @pl.when(even)
                def _():
                    for dt in range(1, T):
                        pass_on(m, src, gg, t, tp=lax.rem(t + dt, T))

            for dt in range(1, T):
                tt = lax.rem(t + dt, T)
                wait_piece(m, src, g, tt)

                @pl.when(jnp.logical_not(even))
                def _():
                    for dg in range(1, G):
                        pass_on(m, src, g, tt, grp=lax.rem(g + dg, G))

    def chain(low, high):
        @pl.loop(low, high)
        def _(d):
            @pl.when(z >= d)
            def _():
                src = f - 2 * d
                tok_copy(block_of(src), src, 2).wait_recv()

                @pl.when(z < Z - 1)
                def _():
                    tok_copy(block_of(src), src, 0).start()

                tok_copy(block_of(src), src, 2).start()

            @pl.when(z + d < Z)
            def _():
                src = f + 2 * d
                tok_copy(block_of(src), src, 2).wait_recv()

                @pl.when(z > 0)
                def _():
                    tok_copy(block_of(src), src, 1).start()

                tok_copy(block_of(src), src, 2).start()

    phase1(0)
    phase1(1)
    phase2(0)
    phase1(2)
    chain(1, 2)
    phase2(1)
    chain(2, 3)
    phase2(2)
    chain(3, Z)

    for m in range(3):

        @pl.loop(0, F)
        def _(src, m=m):
            for dg in range(1, G):
                for dt in range(1, T):
                    wait_piece(m, src, lax.rem(g + dg, G), lax.rem(t + dt, T))

        out = mats[m][1]
        sent = out.at[pl.ds(0, out.shape[0] - mats[m][0].shape[1] // G)]
        remote(sent, sent, send_w.at[m], recv_w.at[m, 0, 0, 0], fs=lax.rem(f + 1, F)).wait_send()

    own[0].wait()
    own_scale.wait()

    @pl.loop(1, F)
    def _(s):
        to = lax.rem(f + s, F)
        scale_copy(to, to).wait_recv()
        scale_copy(to, f).wait_send()

    @pl.loop(0, Z)
    def _(zz):
        src = 2 * zz + core
        other = 2 * zz + 1 - core
        tok_copy(block_of(other), other, 2).wait_recv()
        tok_copy(block_of(src), src, 2).wait_send()

        @pl.when(jnp.logical_and(zz <= z, z < Z - 1))
        def _():
            tok_copy(block_of(src), src, 0).wait_send()

        @pl.when(jnp.logical_and(zz >= z, z > 0))
        def _():
            tok_copy(block_of(src), src, 1).wait_send()


def gathered(mesh, scale_in, tok_in, gate_in, up_in, down_in):
    G, F, T = (mesh.shape[name] for name in ("grp", "fs", "tp"))
    full = [
        jax.ShapeDtypeStruct((T * F * w.shape[1], w.shape[2]), w.dtype)
        for w in (gate_in, up_in, down_in)
    ]
    return pl.pallas_call(
        functools.partial(exchange, (G, F, T)),
        out_shape=[jax.ShapeDtypeStruct(scale_in.shape, scale_in.dtype)]
        + [jax.ShapeDtypeStruct((F * tok_in.shape[0], tok_in.shape[1]), tok_in.dtype)]
        + full,
        in_specs=[pl.BlockSpec(memory_space=pl.ANY)] * 5,
        out_specs=[pl.BlockSpec(memory_space=pltpu.VMEM)] * 5,
        scratch_shapes=[
            pltpu.SemaphoreType.DMA((3, F, G, T)),
            pltpu.SemaphoreType.DMA((3,)),
            pltpu.SemaphoreType.DMA((F,)),
            pltpu.SemaphoreType.DMA((F,)),
            pltpu.SemaphoreType.DMA((F,)),
            pltpu.SemaphoreType.DMA((F,)),
            pltpu.SemaphoreType.DMA((F,)),
            pltpu.SemaphoreType.DMA((F,)),
            pltpu.SemaphoreType.DMA((5,)),
        ],
        compiler_params=pltpu.CompilerParams(
            collective_id=0, has_side_effects=True, vmem_limit_bytes=40 * 1024 * 1024
        ),
    )(scale_in, tok_in, gate_in, up_in, down_in)


def shards(mesh, prompt, routes, route_weight, norm_gain, gate_train, up_train, down_train):
    T = mesh.shape["tp"]
    t = lax.axis_index("tp")
    experts = gate_train.shape[0]
    tok_rows, width = prompt.shape
    part = tok_rows // T
    values = lax.dynamic_slice_in_dim(prompt, t * part, part, 0).astype(jnp.float32)
    normed = (values * lax.rsqrt(jnp.mean(values * values, axis=-1, keepdims=True) + EPS)).astype(
        jnp.bfloat16
    )
    lanes = jnp.arange(experts, dtype=jnp.int32)
    routes = lax.dynamic_slice_in_dim(routes, t * part, part, 0)
    route_weight = lax.dynamic_slice_in_dim(route_weight, t * part, part, 0)
    scale = jnp.sum(
        jnp.where(routes[:, :, None] == lanes[None, None, :], route_weight[:, :, None], 0.0), axis=1
    )

    gain = norm_gain[None, :, None]
    scale, tokens, gate, up, down = gathered(
        mesh,
        scale.T.reshape(experts, 1, part),
        normed,
        (gain * gate_train).astype(jnp.bfloat16),
        (gain * up_train).astype(jnp.bfloat16),
        down_train.astype(jnp.bfloat16),
    )
    scale = scale.reshape(-1, 1)
    gate, up, down = (w.reshape(T, w.shape[0] // T, w.shape[1]) for w in (gate, up, down))
    own = gate.shape[2]
    gate_mine = lax.dynamic_slice_in_dim(gate, t, 1, 0)
    up_mine = lax.dynamic_slice_in_dim(up, t, 1, 0)
    down_mine = lax.dynamic_slice_in_dim(down, t * own, own, 1)
    down_mine = down_mine.transpose(1, 0, 2).reshape(1, own, -1)

    hidden = []
    for i in range(T):
        gate_pre = jnp.dot(tokens, gate[i], preferred_element_type=jnp.float32)
        up_pre = jnp.dot(tokens, up[i], preferred_element_type=jnp.float32)
        gate_pre = jnp.minimum(gate_pre, LIMIT)
        up_pre = jnp.clip(up_pre, -LIMIT, LIMIT)
        hidden.append(
            ((up_pre + 1.0) * gate_pre * jax.nn.sigmoid(ALPHA * gate_pre)).astype(jnp.bfloat16)
        )
    hidden = jnp.concatenate(hidden, axis=1)
    weighted = [
        (jnp.dot(hidden, down[i], preferred_element_type=jnp.float32) * scale).astype(jnp.bfloat16)
        for i in range(T)
    ]
    summed = jnp.stack(
        [lax.psum_scatter(w, "fs", scatter_dimension=0, tiled=True) for w in weighted]
    )
    summed, gate_mine, up_mine, down_mine = lax.optimization_barrier(
        (summed, gate_mine, up_mine, down_mine)
    )
    mixed = lax.all_to_all(summed, "tp", split_axis=0, concat_axis=0, tiled=True)
    mixed = mixed.reshape(tok_rows, -1)
    return (gate_mine, up_mine, down_mine, mixed)


def solution(mesh):
    return jax.shard_map(
        functools.partial(shards, mesh),
        mesh=mesh,
        in_specs=(
            P(("grp", "fs"), None),
            P(("grp", "fs"), None),
            P(("grp", "fs"), None),
            P("fs"),
            P(None, "fs", "tp"),
            P(None, "fs", "tp"),
            P(None, "fs", "tp"),
        ),
        out_specs=(
            P(("grp", "fs"), None, "tp"),
            P(("grp", "fs"), None, "tp"),
            P(("grp", "fs"), "tp", None),
            P(("grp", "fs"), "tp"),
        ),
        check_vma=False,
    )
```
